128 devices in a mesh: ep: 64 (over z, y, x), tp: 2 (over core).
Axes of the slice: x: 4, y: 4, z: 4, core: 2. Of those that a mesh axis runs over, the one named last changes fastest.
Arguments:
- tokens: bfloat16 [256, 1024], P('ep'), may hold values from -6 to 6
- mixer_gain: float32 [1024], replicated, may hold values from 0.1 to 1.9
- w_query: bfloat16 [1024, 2048], P(None, 'tp'), may hold values from -0.1875 to 0.1875
- w_key: bfloat16 [1024, 2048], P(None, 'tp'), may hold values from -0.1875 to 0.1875
- w_value: bfloat16 [1024, 2048], P(None, 'tp'), may hold values from -0.1875 to 0.1875
- w_input_gate: bfloat16 [1024, 4], P(None, 'tp'), may hold values from -0.1875 to 0.1875
- w_forget_gate: bfloat16 [1024, 4], P(None, 'tp'), may hold values from -0.1875 to 0.1875
- forget_bias: float32 [4], P('tp'), may hold values from -1 to 3
- w_output: bfloat16 [2048, 1024], P('tp'), may hold values from -0.125 to 0.125
- memory: float32 [256, 4, 512, 512], P('ep', 'tp'), may hold values from -0.26516503 to 0.26516503
- normalizer: float32 [256, 4, 512], P('ep', 'tp'), may hold values from -0.26516503 to 0.26516503
- stabilizer: float32 [256, 4], P('ep', 'tp'), may hold values from -2 to 2
- ffn_gain: float32 [1024], replicated, may hold values from 0.1 to 1.9
- route_ids: int32 [256, 2], P('ep'), may hold values from 0 to 7, all different within a row; in each aligned block of 4 rows (0 to 3, 4 to 7, ...) at most 2 rows name the same one
- route_weights: float32 [256, 2], P('ep'), may hold values from 0.1 to 1
- expert_gate: bfloat16 [64, 1024, 704], P('ep', None, 'tp'), may hold values from -0.1875 to 0.1875
- expert_up: bfloat16 [64, 1024, 704], P('ep', None, 'tp'), may hold values from -0.1875 to 0.1875
- expert_down: bfloat16 [64, 704, 1024], P('ep', 'tp'), may hold values from -0.078125 to 0.078125
- dense_gate_w: bfloat16 [1024, 4096], P(None, ('ep', 'tp')), may hold values from -0.1875 to 0.1875
- dense_up_w: bfloat16 [1024, 4096], P(None, ('ep', 'tp')), may hold values from -0.1875 to 0.1875
- dense_down_w: bfloat16 [4096, 1024], P(('ep', 'tp')), may hold values from -0.09375 to 0.09375
- dense_scale: float32 [1024], P('tp'), may hold values from 0.3 to 1.5
Outputs:
- output: bfloat16 [256, 1024], P('ep', 'tp')
- new_memory: float32 [256, 4, 512, 512], P('ep', 'tp')
- new_normalizer: float32 [256, 4, 512], P('ep', 'tp')
- new_stabilizer: float32 [256, 4], P('ep', 'tp')
The draws below stay inside these ranges and needn't reach their ends.
Inputs may be any that keep to these rules, and one draw needn't show every extreme that they name: `route_ids`: the two experts of a row differ. In each aligned block of 4 rows (the rows of one device group) no expert is named by more than 2 rows, a bound that some block reaches.
All inputs are finite; a program needn't handle non-finite values.
Results may differ from the reference program's by a relative error of at most 0.015.
Values may be sent and summed in bfloat16 or wider, within the bound.
A program may use at most 128 MiB of HBM per device.

```python
import math
import jax
import jax.numpy as jnp
import numpy as np
from jax import lax

D = 1024
HEADS = 4
HEAD_SIZE = 512
INNER = 2048
EXPERTS = 8
TOP_K = 2
EXPERT_HIDDEN = 5632
DENSE_HIDDEN = 4096
GROUP_SEQS = 4
CAPACITY = 2
EXPERT_SPLIT = 8
TOKENS = 256


def steps_of(own_key, extent, cuts, smallest, high):
    def one(axis_at, shards_of):
        heights = jax.random.uniform(jax.random.fold_in(jax.random.fold_in(own_key, 6), axis_at), (shards_of,), jnp.float32, smallest / len(cuts), high / len(cuts))
        return jnp.repeat(jnp.exp(heights), extent[axis_at] // shards_of).reshape((-1,) + (1,) * (len(extent) - axis_at - 1))

    level = one(*cuts[0])
    for cut in cuts[1:]:
        level = level * one(*cut)
    return level


def assign_block(own_key, own, number, rows, count, top, most, slope):
    ranking = jax.random.permutation(own_key, count)
    heavy_load, usual = portions_of(count, rows * top, most, slope, True), portions_of(count, rows * top, most, slope, False)
    places = jnp.arange(count)

    def named(lengths, offset_by):
        used = int((lengths > 0).sum())
        fixed = max(1, used // 4)
        passed = fixed + (places - fixed + offset_by * (used - fixed)) % max(1, count - fixed)
        return jnp.zeros((count,), jnp.int32).at[ranking[jnp.where(places < fixed, places, passed)]].set(jnp.asarray(lengths, jnp.int32))

    lengths = jnp.where(number % 4 == 0, named(heavy_load, number // 4), named(usual, number - number // 4 - 1))
    mixed = jax.random.permutation(jax.random.fold_in(own, 3), count)
    giver, taker = mixed[0:count // 2 * 2:2], mixed[1:count // 2 * 2:2]
    margin = jnp.minimum(lengths[giver] - 1, most - lengths[taker]) // 2
    margin = jnp.where((giver == ranking[0]) | (taker == ranking[0]) | (lengths[taker] == 0), 0, jnp.maximum(margin, 0))
    passed = jax.random.randint(jax.random.fold_in(own, 4), (count // 2,), 0, 1 << 20) % (margin + 1)
    lengths = lengths.at[giver].add(-passed).at[taker].add(passed)
    members = jnp.searchsorted(jnp.cumsum(lengths), jnp.arange(rows * top), side="right").astype(jnp.int32)
    table = members.reshape(top, rows).T
    table = table[jax.random.permutation(jax.random.fold_in(own, 1), rows)]
    offset_by = jax.random.randint(jax.random.fold_in(own, 2), (rows, 1), 0, top)
    return jnp.take_along_axis(table, (jnp.arange(top)[None, :] + offset_by) % top, axis=1)


def portions_of(number_of, total, most, slope, full):
    portions = [(1 << 20) // math.isqrt(grade ** slope) + 1 for grade in range(1, number_of + 1)]
    largest = most if full else min(most, max(-(-total // number_of), total * portions[0] // sum(portions)))
    least = 1 if total - largest >= number_of - 1 else 0
    holding, surplus = [largest] + [least] * (number_of - 1), total - largest - least * (number_of - 1)
    while surplus > 0:
        free = [i for i in range(1, number_of) if holding[i] < largest] or [i for i in range(1, number_of) if holding[i] < most]
        pool, left = sum([portions[i] for i in free]), surplus
        for i in free:
            more = min(most - holding[i], max(1, left * portions[i] // pool), surplus)
            holding[i] = holding[i] + more
            surplus = surplus - more
    return np.array(holding)


def noise(key, extent, deviation, most, pieces=(), held_as=jnp.bfloat16):
    values = jax.random.normal(key, extent, jnp.float32) * deviation
    if len(pieces) > 0:
        values = steps_of(key, extent, pieces, -0.22, 0.18) * values
    return jnp.clip(values, min=-most, max=most).astype(held_as)


def setup_inputs(seed: int = 0) -> dict:
    keys = jax.random.split(jax.random.key(seed), 23)
    tokens = noise(keys[0], (TOKENS, D), 1.0, 6.0, ((0, 64),))
    mixer_gain = jnp.clip(1.0 + 0.18 * jax.random.normal(keys[1], (D,), jnp.float32), 0.1, 1.9)
    w_query = noise(keys[2], (D, INNER), D ** -0.5, 0.1875, ((1, 2),))
    w_key = noise(keys[3], (D, INNER), D ** -0.5, 0.1875, ((1, 2),))
    w_value = noise(keys[4], (D, INNER), D ** -0.5, 0.1875, ((1, 2),))
    w_input_gate = noise(keys[5], (D, HEADS), D ** -0.5, 0.1875, ((1, 2),))
    w_forget_gate = noise(keys[6], (D, HEADS), D ** -0.5, 0.1875, ((1, 2),))
    forget_bias = jnp.clip(-1.0 + 4.0 * jax.random.uniform(keys[7], (HEADS,), jnp.float32) ** steps_of(keys[7], (HEADS,), ((0, 2),), -0.2, 0.2), -1.0, 3.0)
    w_output = noise(keys[8], (INNER, D), INNER ** -0.5, 0.125, ((0, 2),))
    memory = noise(keys[9], (TOKENS, HEADS, HEAD_SIZE, HEAD_SIZE), (HEAD_SIZE ** -0.5), 0.26516503, ((0, 64), (1, 2)), jnp.float32)
    normalizer = noise(keys[10], (TOKENS, HEADS, HEAD_SIZE), (HEAD_SIZE ** -0.5), 0.26516503, ((0, 64), (1, 2)), jnp.float32)
    stabilizer = jnp.clip(jax.random.uniform(keys[11], (TOKENS, HEADS), jnp.float32, -2.0, 2.0) * steps_of(keys[11], (TOKENS, HEADS), ((0, 64), (1, 2)), -0.4, 0.0), -2.0, 2.0)
    ffn_gain = jnp.clip(1.0 + 0.18 * jax.random.normal(keys[12], (D,), jnp.float32), 0.1, 1.9)
    route_ids_keys = jax.random.split(jax.random.fold_in(keys[13], 1), TOKENS // GROUP_SEQS)
    route_ids_turns = jax.random.permutation(jax.random.fold_in(keys[13], 3), TOKENS // GROUP_SEQS)
    route_ids = jax.vmap(lambda own, number: assign_block(jax.random.fold_in(keys[13], 2), own, number, GROUP_SEQS, EXPERTS, TOP_K, CAPACITY, 2))(route_ids_keys, route_ids_turns).reshape((TOKENS, TOP_K))
    route_weights = jnp.clip(0.1 + 0.9 * jax.random.uniform(keys[14], (TOKENS, TOP_K), jnp.float32) ** steps_of(keys[14], (TOKENS, TOP_K), ((0, 64),), -0.2, 0.2), 0.1, 1.0)
    expert_gate = noise(keys[15], (EXPERTS * EXPERT_SPLIT, D, EXPERT_HIDDEN // EXPERT_SPLIT), D ** -0.5, 0.1875, ((0, 64), (2, 2)))
    expert_up = noise(keys[16], (EXPERTS * EXPERT_SPLIT, D, EXPERT_HIDDEN // EXPERT_SPLIT), D ** -0.5, 0.1875, ((0, 64), (2, 2)))
    expert_down = noise(keys[17], (EXPERTS * EXPERT_SPLIT, EXPERT_HIDDEN // EXPERT_SPLIT, D), EXPERT_HIDDEN ** -0.5, 0.078125, ((0, 64), (1, 2)))
    dense_gate_w = noise(keys[18], (D, DENSE_HIDDEN), D ** -0.5, 0.1875, ((1, 128),))
    dense_up_w = noise(keys[19], (D, DENSE_HIDDEN), D ** -0.5, 0.1875, ((1, 128),))
    dense_down_w = noise(keys[20], (DENSE_HIDDEN, D), DENSE_HIDDEN ** -0.5, 0.09375, ((0, 128),))
    dense_scale = jnp.clip(0.3 + 1.2 * jax.random.uniform(keys[21], (D,), jnp.float32) ** steps_of(keys[21], (D,), ((0, 2),), -0.2, 0.2), 0.3, 1.5)
    return {"tokens": tokens, "mixer_gain": mixer_gain, "w_query": w_query, "w_key": w_key, "w_value": w_value, "w_input_gate": w_input_gate, "w_forget_gate": w_forget_gate, "forget_bias": forget_bias, "w_output": w_output, "memory": memory, "normalizer": normalizer, "stabilizer": stabilizer, "ffn_gain": ffn_gain, "route_ids": route_ids, "route_weights": route_weights, "expert_gate": expert_gate, "expert_up": expert_up, "expert_down": expert_down, "dense_gate_w": dense_gate_w, "dense_up_w": dense_up_w, "dense_down_w": dense_down_w, "dense_scale": dense_scale}


def normalize(values_in, gain):
    values = values_in.astype(jnp.float32)
    scale = lax.rsqrt(lax.optimization_barrier(jnp.mean(values * values, axis=-1, keepdims=True)) + 1e-06)
    return (values * scale * gain).astype(jnp.bfloat16)

def cell_step(query_heads, key_heads, value_heads, in_gate, forget_log, memory, normalizer, stabilizer):
    new_stabilizer = jnp.maximum(forget_log + stabilizer, in_gate)
    carry = jnp.exp(forget_log + stabilizer - new_stabilizer)
    admit = jnp.exp(in_gate - new_stabilizer)
    scaled_key = admit[..., None] * key_heads
    new_memory = carry[..., None, None] * memory + scaled_key[..., :, None] * value_heads[..., None, :]
    new_normalizer = carry[..., None] * normalizer + scaled_key
    numer = jnp.einsum('...hd,...hde->...he', query_heads, new_memory, precision=lax.Precision.HIGHEST)
    denom = lax.optimization_barrier(jnp.sum(new_normalizer * query_heads, axis=-1))
    bound = jnp.maximum(jnp.abs(denom), jnp.exp(-new_stabilizer))
    return (numer / bound[..., None], new_memory, new_normalizer, new_stabilizer)

def reference(tokens, mixer_gain, w_query, w_key, w_value, w_input_gate, w_forget_gate, forget_bias, w_output, memory, normalizer, stabilizer, ffn_gain, route_ids, route_weights, expert_gate, expert_up, expert_down, dense_gate_w, dense_up_w, dense_down_w, dense_scale):
    normed = normalize(tokens, mixer_gain)
    query = jnp.dot(normed, w_query, preferred_element_type=jnp.float32).astype(jnp.bfloat16)
    key = jnp.dot(normed, w_key, preferred_element_type=jnp.float32).astype(jnp.bfloat16)
    value = jnp.dot(normed, w_value, preferred_element_type=jnp.float32).astype(jnp.bfloat16)
    in_gate = jnp.dot(normed, w_input_gate, preferred_element_type=jnp.float32)
    forget_log = jax.nn.log_sigmoid(jnp.dot(normed, w_forget_gate, preferred_element_type=jnp.float32) + forget_bias)
    shaped = (TOKENS, HEADS, HEAD_SIZE)
    query_heads = query.astype(jnp.float32).reshape(shaped)
    key_heads = key.astype(jnp.float32).reshape(shaped) * HEAD_SIZE ** (-0.5)
    value_heads = value.astype(jnp.float32).reshape(shaped)

    def per_token(inputs):
        return cell_step(*inputs)
    read, new_memory, new_normalizer, new_stabilizer = lax.map(per_token, (query_heads, key_heads, value_heads, in_gate, forget_log, memory, normalizer, stabilizer))
    read = read.reshape(TOKENS, INNER).astype(jnp.bfloat16)
    half_cols = INNER // 2
    first = jnp.dot(read[:, :half_cols], w_output[:half_cols], preferred_element_type=jnp.float32)
    second = jnp.dot(read[:, half_cols:], w_output[half_cols:], preferred_element_type=jnp.float32)
    first = lax.optimization_barrier(first.astype(jnp.bfloat16)).astype(jnp.float32)
    second = lax.optimization_barrier(second.astype(jnp.bfloat16)).astype(jnp.float32)
    stream = tokens.astype(jnp.float32) + (first + second)
    ffn_in = normalize(stream, ffn_gain)
    block_units = EXPERT_HIDDEN // EXPERT_SPLIT
    gate_full = expert_gate.reshape(EXPERTS, EXPERT_SPLIT, D, block_units).transpose(0, 2, 1, 3).reshape(EXPERTS, D, EXPERT_HIDDEN)
    up_full = expert_up.reshape(EXPERTS, EXPERT_SPLIT, D, block_units).transpose(0, 2, 1, 3).reshape(EXPERTS, D, EXPERT_HIDDEN)
    down_full = expert_down.reshape(EXPERTS, EXPERT_HIDDEN, D)

    def one_expert(total, inputs):
        gate_matrix, up_matrix, down_matrix, expert_id = inputs
        column = lax.optimization_barrier(jnp.sum(route_weights * (route_ids == expert_id).astype(jnp.float32), axis=1))
        gated = jnp.dot(ffn_in, gate_matrix, preferred_element_type=jnp.float32)
        lifted = jnp.dot(ffn_in, up_matrix, preferred_element_type=jnp.float32)
        hidden = (jax.nn.silu(gated) * lifted).astype(jnp.bfloat16)
        result = jnp.dot(hidden, down_matrix, preferred_element_type=jnp.float32)
        return (total + column[:, None] * result, None)
    routed, unused = lax.scan(one_expert, jnp.zeros((TOKENS, D), jnp.float32), (gate_full, up_full, down_full, jnp.arange(EXPERTS, dtype=jnp.int32)))
    dense_gated = jnp.dot(ffn_in, dense_gate_w, preferred_element_type=jnp.float32)
    dense_lifted = jnp.dot(ffn_in, dense_up_w, preferred_element_type=jnp.float32)
    dense_hidden = (jax.nn.silu(dense_gated) * dense_lifted).astype(jnp.bfloat16)
    dense = jnp.dot(dense_hidden, dense_down_w, preferred_element_type=jnp.float32)
    output = (stream + routed + dense_scale * dense).astype(jnp.bfloat16)
    return (output, new_memory, new_normalizer, new_stabilizer)
```

```python
import functools

import jax
import jax.numpy as jnp
from jax import lax
from jax.experimental import pallas as pl
from jax.experimental.pallas import tpu as pltpu
from jax.sharding import PartitionSpec as P

EXPERTS = 8
RING = 4
PLANE = 16
ROWS = 4
BLOCK = 16
TOKENS = 256
WIDTH = 1024
HALF = 512
UNITS = 352
DENSE = 32
ALL_UNITS = 384
MESH = pl.DeviceIdType.MESH
F32 = jnp.float32
BF16 = jnp.bfloat16
EPSILON = 1e-06
OFFSETS = sorted(
    [(dz, dy) for dz in range(RING) for dy in range(RING) if (dz, dy) != (0, 0)],
    key=lambda o: -(min(o[0], RING - o[0]) + min(o[1], RING - o[1])),
)


def normalize(values_in, gain):
    values = values_in.astype(F32)
    scale = lax.rsqrt(jnp.mean(values * values, axis=-1, keepdims=True) + EPSILON)
    return (values * scale * gain).astype(BF16)


def ffn_kernel(
    tokens_ref,
    partial_ref,
    gain_ref,
    ids_ref,
    weights_ref,
    scale_ref,
    gate_hbm,
    up_hbm,
    down_hbm,
    dense_gate_hbm,
    dense_up_hbm,
    dense_down_hbm,
    out_ref,
    other_partial,
    scales,
    stream,
    own_rows,
    row_in,
    weight_row,
    weight_in,
    gathered,
    weight_table,
    w_in,
    w_down,
    part_out,
    part_in,
    part_own,
    block_out,
    block_in,
    piece_out,
    piece_in,
    load_sem,
    pair_send,
    pair_recv,
    row_send,
    row_recv,
    plane_send,
    plane_recv,
    share_send,
    share_recv,
    sum_send,
    sum_recv,
    back_send,
    back_recv,
    piece_send,
    piece_recv,
):
    chip = lax.axis_index("ep")
    core = lax.axis_index("tp")
    other = 1 - core
    place = chip // RING
    x = lax.rem(chip, RING)
    z, y = place // RING, lax.rem(place, RING)

    def to(chip_at, core_at):
        return {"ep": chip_at, "tp": core_at}

    def plane_at(dz, dy):
        return lax.rem(z + dz, RING) * RING + lax.rem(y + dy, RING)

    def send(src, dst, send_sem, recv_sem, chip_at, core_at):
        copy = pltpu.make_async_remote_copy(
            src_ref=src,
            dst_ref=dst,
            send_sem=send_sem,
            recv_sem=recv_sem,
            device_id=to(chip_at, core_at),
            device_id_type=MESH,
        )
        copy.start()
        return copy

    barrier = pltpu.get_barrier_semaphore()
    pl.semaphore_signal(barrier, inc=1, device_id=to(chip, other), device_id_type=MESH)
    for d in range(1, RING):
        pl.semaphore_signal(
            barrier,
            inc=1,
            device_id=to(place * RING + lax.rem(x + d, RING), core),
            device_id_type=MESH,
        )
    for dz, dy in OFFSETS:
        pl.semaphore_signal(
            barrier,
            inc=1,
            device_id=to(plane_at(dz, dy) * RING + x, core),
            device_id_type=MESH,
        )

    loads = [
        (gate_hbm, w_in.at[pl.ds(0, UNITS)]),
        (dense_gate_hbm, w_in.at[pl.ds(UNITS, DENSE)]),
        (up_hbm, w_in.at[pl.ds(ALL_UNITS, UNITS)]),
        (dense_up_hbm, w_in.at[pl.ds(ALL_UNITS + UNITS, DENSE)]),
        (down_hbm.at[:, pl.ds(0, HALF)], w_down.at[0, pl.ds(0, UNITS)]),
        (down_hbm.at[:, pl.ds(HALF, HALF)], w_down.at[1, pl.ds(0, UNITS)]),
        (dense_down_hbm.at[:, pl.ds(0, HALF)], w_down.at[0, pl.ds(UNITS, DENSE)]),
        (dense_down_hbm.at[:, pl.ds(HALF, HALF)], w_down.at[1, pl.ds(UNITS, DENSE)]),
    ]
    loading = []
    for i, (src, dst) in enumerate(loads):
        copy = pltpu.make_async_copy(src, dst, load_sem.at[i])
        copy.start()
        loading.append(copy)

    pl.semaphore_wait(barrier, 1 + RING - 1 + PLANE - 1)

    pending = []
    pair = [
        send(partial_ref, other_partial, pair_send.at[0], pair_recv.at[0], chip, other),
        send(scale_ref, scales.at[core], pair_send.at[1], pair_recv.at[1], chip, other),
    ]
    scales[core] = scale_ref[...]
    lane = lax.broadcasted_iota(jnp.int32, (1, 128), 1)
    row = jnp.zeros((1, 128), F32)
    for i in range(ROWS):
        for k in range(2):
            hit = lane == x * (ROWS * EXPERTS) + i * EXPERTS + ids_ref[k, i]
            row = row + jnp.where(hit, weights_ref[k, i], 0.0)
    weight_row[...] = row
    for d in range(1, RING):
        q = place * RING + lax.rem(x + d, RING)
        pending.append(
            send(weight_row, weight_in.at[d], row_send.at[1, d], row_recv.at[1, d], q, core)
        )
    pair[0].wait_recv()
    mixed = partial_ref[...].astype(F32) + other_partial[...].astype(F32)
    total = tokens_ref[...].astype(F32) + mixed
    stream[0] = total[:, :HALF]
    stream[1] = total[:, HALF:]
    ffn_in = normalize(total, gain_ref[...])
    own_rows[0] = ffn_in[:, :HALF]
    own_rows[1] = ffn_in[:, HALF:]
    for d in range(1, RING):
        q = place * RING + lax.rem(x + d, RING)
        pending.append(
            send(own_rows.at[core], row_in.at[x], row_send.at[0, d], row_recv.at[0, d], q, core)
        )
    row_in[x] = own_rows[core]
    for d in range(1, RING):
        pending[d - 1].wait_recv()
        row = row + weight_in[d]
    weight_table[pl.ds(place, 1), :] = row
    for d in range(1, RING):
        pending[RING - 1 + d - 1].wait_recv()
    rows16 = jnp.concatenate([row_in[j].astype(F32) for j in range(RING)], axis=0)
    own_block = gathered.at[core, pl.ds(pl.multiple_of(place * BLOCK, BLOCK), BLOCK)]
    own_block[...] = rows16.astype(BF16)

    arriving = []
    for i, (dz, dy) in enumerate(OFFSETS):
        q = plane_at(dz, dy) * RING + x
        arriving.append(
            (
                send(own_block, own_block, plane_send.at[0, i], plane_recv.at[0, i], q, core),
                send(
                    weight_table.at[pl.ds(place, 1)],
                    weight_table.at[pl.ds(place, 1)],
                    plane_send.at[1, i],
                    plane_recv.at[1, i],
                    q,
                    core,
                ),
            )
        )
    shared = [send(own_block, own_block, share_send.at[PLANE - 1], share_recv.at[PLANE - 1], chip, other)]
    for i in reversed(range(PLANE - 1)):
        dz, dy = OFFSETS[i]
        arriving[i][0].wait_recv()
        came = plane_at(RING - dz, RING - dy)
        block = gathered.at[core, pl.ds(pl.multiple_of(came * BLOCK, BLOCK), BLOCK)]
        shared.append(send(block, block, share_send.at[i], share_recv.at[i], chip, other))

    for copy in loading:
        copy.wait()
    pair[1].wait_recv()
    for half in range(2):
        w_down[half, UNITS:, :] = (
            w_down[half, UNITS:, :].astype(F32) * scales[half]
        ).astype(BF16)
    for i in range(PLANE - 1):
        arriving[i][1].wait_recv()
    expert = chip // EXPERTS
    sub = lax.broadcasted_iota(jnp.int32, (BLOCK, 128), 0)
    lane16 = lax.broadcasted_iota(jnp.int32, (BLOCK, 128), 1)
    picked = lane16 == sub * EXPERTS + expert
    table = weight_table[...]
    columns = [
        jnp.sum(jnp.where(picked, table[g : g + 1, :], 0.0), axis=1, keepdims=True)
        for g in range(PLANE)
    ]
    column = jnp.concatenate(columns, axis=0)

    for copy in shared:
        copy.wait_recv()
    nt = (((1,), (1,)), ((), ()))
    raised = lax.dot_general(
        gathered[0], w_in[:, :HALF], nt, preferred_element_type=F32
    ) + lax.dot_general(gathered[1], w_in[:, HALF:], nt, preferred_element_type=F32)
    gated = raised[:, :ALL_UNITS]
    lifted = raised[:, ALL_UNITS:]
    unit = lax.broadcasted_iota(jnp.int32, (TOKENS, ALL_UNITS), 1)
    hidden = gated / (1.0 + jnp.exp(-gated)) * lifted * jnp.where(unit < UNITS, column, 1.0)
    hidden = hidden.astype(BF16)
    part_out[...] = jnp.dot(hidden, w_down[other], preferred_element_type=F32).astype(BF16)
    swap = send(part_out, part_in, sum_send.at[0], sum_recv.at[0], chip, other)
    part_own[...] = jnp.dot(hidden, w_down[core], preferred_element_type=F32)
    swap.wait_recv()
    summed = part_own[...] + part_in[...].astype(F32)
    block_out[...] = summed.astype(BF16)
    part_own[...] = summed
    back = []
    for i, (dz, dy) in enumerate(OFFSETS):
        q = plane_at(dz, dy)
        block = block_out.at[pl.ds(pl.multiple_of(q * BLOCK, BLOCK), BLOCK)]
        back.append(
            send(block, block_in.at[i], back_send.at[i], back_recv.at[i], q * RING + x, core)
        )
    total = part_own[pl.ds(pl.multiple_of(place * BLOCK, BLOCK), BLOCK), :]
    for i in reversed(range(PLANE - 1)):
        back[i].wait_recv()
        total = total + block_in[i].astype(F32)
    for j in range(RING):
        piece_out[j] = total[j * ROWS : (j + 1) * ROWS, :].astype(BF16)
    pieces = []
    for d in range(1, RING):
        at = lax.rem(x + d, RING)
        pieces.append(
            send(
                piece_out.at[at],
                piece_in.at[d],
                piece_send.at[d],
                piece_recv.at[d],
                place * RING + at,
                core,
            )
        )
    result = stream[core] + piece_out[x].astype(F32)
    for copy in pieces:
        copy.wait_recv()
    for d in range(1, RING):
        result = result + piece_in[d].astype(F32)
    out_ref[...] = result.astype(BF16)

    for copy in pair + pending + shared + [swap] + back + pieces:
        copy.wait_send()
    for a, b in arriving:
        a.wait_send()
        b.wait_send()


def ffn(tokens, partial, ffn_gain, ids, weights, scale, gate, up, down, dense_gate, dense_up, dense_down):
    vmem = pl.BlockSpec(memory_space=pltpu.VMEM)
    smem = pl.BlockSpec(memory_space=pltpu.SMEM)
    hbm = pl.BlockSpec(memory_space=pl.ANY)
    dma = pltpu.SemaphoreType.DMA
    return pl.pallas_call(
        ffn_kernel,
        out_shape=jax.ShapeDtypeStruct((ROWS, HALF), BF16),
        in_specs=[vmem, vmem, vmem, smem, smem, vmem] + [hbm] * 6,
        out_specs=vmem,
        scratch_shapes=[
            pltpu.VMEM((ROWS, WIDTH), BF16),
            pltpu.VMEM((2, 1, HALF), F32),
            pltpu.VMEM((2, ROWS, HALF), F32),
            pltpu.VMEM((2, ROWS, HALF), BF16),
            pltpu.VMEM((RING, ROWS, HALF), BF16),
            pltpu.VMEM((1, 128), F32),
            pltpu.VMEM((RING, 1, 128), F32),
            pltpu.VMEM((2, TOKENS, HALF), BF16),
            pltpu.VMEM((PLANE, 128), F32),
            pltpu.VMEM((2 * ALL_UNITS, WIDTH), BF16),
            pltpu.VMEM((2, ALL_UNITS, HALF), BF16),
            pltpu.VMEM((TOKENS, HALF), BF16),
            pltpu.VMEM((TOKENS, HALF), BF16),
            pltpu.VMEM((TOKENS, HALF), F32),
            pltpu.VMEM((TOKENS, HALF), BF16),
            pltpu.VMEM((PLANE, BLOCK, HALF), BF16),
            pltpu.VMEM((RING, ROWS, HALF), BF16),
            pltpu.VMEM((RING, ROWS, HALF), BF16),
            dma((8,)),
            dma((2,)),
            dma((2,)),
            dma((2, RING)),
            dma((2, RING)),
            dma((2, PLANE)),
            dma((2, PLANE)),
            dma((PLANE,)),
            dma((PLANE,)),
            dma((1,)),
            dma((1,)),
            dma((PLANE,)),
            dma((PLANE,)),
            dma((RING,)),
            dma((RING,)),
        ],
        compiler_params=pltpu.CompilerParams(
            collective_id=0, has_side_effects=True, vmem_limit_bytes=32 * 2**20
        ),
    )(tokens, partial, ffn_gain, ids, weights, scale, gate, up, down, dense_gate, dense_up, dense_down)


def cell_step(
    query_heads, key_heads, value_heads, in_gate, forget_log, memory, normalizer, stabilizer
):
    new_stabilizer = jnp.maximum(forget_log + stabilizer, in_gate)
    carry = jnp.exp(forget_log + stabilizer - new_stabilizer)
    admit = jnp.exp(in_gate - new_stabilizer)
    scaled_key = admit[..., None] * key_heads
    new_memory = (
        carry[..., None, None] * memory + scaled_key[..., :, None] * value_heads[..., None, :]
    )
    new_normalizer = carry[..., None] * normalizer + scaled_key
    numer = jnp.einsum(
        "...hd,...hde->...he", query_heads, new_memory, precision=lax.Precision.HIGHEST
    )
    denom = jnp.sum(new_normalizer * query_heads, axis=-1)
    bound = jnp.maximum(jnp.abs(denom), jnp.exp(-new_stabilizer))
    return (numer / bound[..., None], new_memory, new_normalizer, new_stabilizer)


def shards(
    tokens,
    mixer_gain,
    w_query,
    w_key,
    w_value,
    w_input_gate,
    w_forget_gate,
    forget_bias,
    w_output,
    memory,
    normalizer,
    stabilizer,
    ffn_gain,
    route_ids,
    route_weights,
    expert_gate,
    expert_up,
    expert_down,
    dense_gate_w,
    dense_up_w,
    dense_down_w,
    dense_scale,
):
    local_rows = tokens.shape[0]
    local_heads = memory.shape[1]
    head_size = memory.shape[2]
    width = tokens.shape[1]
    normed = normalize(tokens, mixer_gain)
    query = jnp.dot(normed, w_query, preferred_element_type=jnp.float32).astype(jnp.bfloat16)
    key = jnp.dot(normed, w_key, preferred_element_type=jnp.float32).astype(jnp.bfloat16)
    value = jnp.dot(normed, w_value, preferred_element_type=jnp.float32).astype(jnp.bfloat16)
    in_gate = jnp.dot(normed, w_input_gate, preferred_element_type=jnp.float32)
    forget_log = jax.nn.log_sigmoid(
        jnp.dot(normed, w_forget_gate, preferred_element_type=jnp.float32) + forget_bias
    )
    shaped = (local_rows, local_heads, head_size)
    query_heads = query.astype(jnp.float32).reshape(shaped)
    key_heads = key.astype(jnp.float32).reshape(shaped) * head_size ** (-0.5)
    value_heads = value.astype(jnp.float32).reshape(shaped)
    read, new_memory, new_normalizer, new_stabilizer = cell_step(
        query_heads, key_heads, value_heads, in_gate, forget_log, memory, normalizer, stabilizer
    )
    read = read.reshape(local_rows, local_heads * head_size).astype(jnp.bfloat16)
    partial_value = jnp.dot(read, w_output, preferred_element_type=jnp.float32)
    output = ffn(
        tokens,
        partial_value.astype(jnp.bfloat16),
        ffn_gain.reshape(1, width),
        route_ids.T,
        route_weights.T,
        dense_scale.reshape(1, -1),
        expert_gate[0].T,
        expert_up[0].T,
        expert_down[0],
        dense_gate_w.T,
        dense_up_w.T,
        dense_down_w,
    )
    return (output, new_memory, new_normalizer, new_stabilizer)


def solution(mesh):
    placed = (
        P("ep", None),
        P(),
        P(None, "tp"),
        P(None, "tp"),
        P(None, "tp"),
        P(None, "tp"),
        P(None, "tp"),
        P("tp"),
        P("tp", None),
        P("ep", "tp", None, None),
        P("ep", "tp", None),
        P("ep", "tp"),
        P(),
        P("ep", None),
        P("ep", None),
        P("ep", None, "tp"),
        P("ep", None, "tp"),
        P("ep", "tp", None),
        P(None, ("ep", "tp")),
        P(None, ("ep", "tp")),
        P(("ep", "tp"), None),
        P("tp"),
    )
    return jax.shard_map(
        shards,
        mesh=mesh,
        in_specs=placed,
        out_specs=(P("ep", "tp"), P("ep", "tp", None, None), P("ep", "tp", None), P("ep", "tp")),
        check_vma=False,
    )
```

```python
import functools

import jax
import jax.numpy as jnp
from jax import lax
from jax.experimental import pallas as pl
from jax.experimental.pallas import tpu as pltpu
from jax.sharding import PartitionSpec as P

EXPERTS = 8
RING = 4
PLANE = 16
ROWS = 4
BLOCK = 16
TOKENS = 256
WIDTH = 1024
HALF = 512
K2_VMEM = 40 * 2**20
K1_VMEM = 40 * 2**20
UNITS = 352
DENSE = 32
ALL_UNITS = 384
HEADS = 2
HEAD_SIZE = 512
PAIRS = 8
CHUNK = 64
MESH = pl.DeviceIdType.MESH
F32 = jnp.float32
BF16 = jnp.bfloat16
EPSILON = 1e-06
OFFSETS = sorted(
    [(dz, dy) for dz in range(RING) for dy in range(RING) if (dz, dy) != (0, 0)],
    key=lambda o: -(min(o[0], RING - o[0]) + min(o[1], RING - o[1])),
)


def normalize(values_in, gain):
    values = values_in.astype(F32)
    scale = lax.rsqrt(jnp.mean(values * values, axis=-1, keepdims=True) + EPSILON)
    return (values * scale * gain).astype(BF16)


def ffn_kernel(
    tokens_ref,
    read_ref,
    gain_ref,
    ids_ref,
    weights_ref,
    scale_ref,
    output_hbm,
    gate_hbm,
    up_hbm,
    down_hbm,
    dense_gate_hbm,
    dense_up_hbm,
    dense_down_hbm,
    out_ref,
    w_output,
    partial_ref,
    other_partial,
    scales,
    stream,
    own_rows,
    row_in,
    weight_row,
    weight_in,
    gathered,
    weight_table,
    w_in,
    w_down,
    part_out,
    part_in,
    part_own,
    block_out,
    block_in,
    piece_out,
    piece_in,
    load_sem,
    pair_send,
    pair_recv,
    row_send,
    row_recv,
    plane_send,
    plane_recv,
    share_send,
    share_recv,
    sum_send,
    sum_recv,
    back_send,
    back_recv,
    piece_send,
    piece_recv,
):
    chip = lax.axis_index("ep")
    core = lax.axis_index("tp")
    other = 1 - core
    place = chip // RING
    x = lax.rem(chip, RING)
    z, y = place // RING, lax.rem(place, RING)

    def to(chip_at, core_at):
        return {"ep": chip_at, "tp": core_at}

    def plane_at(dz, dy):
        return lax.rem(z + dz, RING) * RING + lax.rem(y + dy, RING)

    def send(src, dst, send_sem, recv_sem, chip_at, core_at):
        copy = pltpu.make_async_remote_copy(
            src_ref=src,
            dst_ref=dst,
            send_sem=send_sem,
            recv_sem=recv_sem,
            device_id=to(chip_at, core_at),
            device_id_type=MESH,
        )
        copy.start()
        return copy

    barrier = pltpu.get_barrier_semaphore()
    pl.semaphore_signal(barrier, inc=1, device_id=to(chip, other), device_id_type=MESH)
    for d in range(1, RING):
        pl.semaphore_signal(
            barrier,
            inc=1,
            device_id=to(place * RING + lax.rem(x + d, RING), core),
            device_id_type=MESH,
        )
    for dz, dy in OFFSETS:
        pl.semaphore_signal(
            barrier,
            inc=1,
            device_id=to(plane_at(dz, dy) * RING + x, core),
            device_id_type=MESH,
        )

    loads = [
        (output_hbm, w_output),
        (gate_hbm, w_in.at[pl.ds(0, UNITS)]),
        (dense_gate_hbm, w_in.at[pl.ds(UNITS, DENSE)]),
        (up_hbm, w_in.at[pl.ds(ALL_UNITS, UNITS)]),
        (dense_up_hbm, w_in.at[pl.ds(ALL_UNITS + UNITS, DENSE)]),
        (down_hbm.at[:, pl.ds(0, HALF)], w_down.at[0, pl.ds(0, UNITS)]),
        (down_hbm.at[:, pl.ds(HALF, HALF)], w_down.at[1, pl.ds(0, UNITS)]),
        (dense_down_hbm.at[:, pl.ds(0, HALF)], w_down.at[0, pl.ds(UNITS, DENSE)]),
        (dense_down_hbm.at[:, pl.ds(HALF, HALF)], w_down.at[1, pl.ds(UNITS, DENSE)]),
    ]
    loading = []
    for i, (src, dst) in enumerate(loads):
        copy = pltpu.make_async_copy(src, dst, load_sem.at[i])
        copy.start()
        loading.append(copy)

    loading[0].wait()
    partial_ref[...] = jnp.dot(
        read_ref[...], w_output[...], preferred_element_type=F32
    ).astype(BF16)
    pl.semaphore_wait(barrier, 1 + RING - 1 + PLANE - 1)

    pending = []
    pair = [
        send(partial_ref, other_partial, pair_send.at[0], pair_recv.at[0], chip, other),
        send(scale_ref, scales.at[core], pair_send.at[1], pair_recv.at[1], chip, other),
    ]
    scales[core] = scale_ref[...]
    lane = lax.broadcasted_iota(jnp.int32, (1, 128), 1)
    row = jnp.zeros((1, 128), F32)
    for i in range(ROWS):
        for k in range(2):
            hit = lane == x * (ROWS * EXPERTS) + i * EXPERTS + ids_ref[k : k + 1, i : i + 1]
            row = row + jnp.where(hit, weights_ref[k : k + 1, i : i + 1], 0.0)
    weight_row[...] = row
    for d in range(1, RING):
        q = place * RING + lax.rem(x + d, RING)
        pending.append(
            send(weight_row, weight_in.at[d], row_send.at[1, d], row_recv.at[1, d], q, core)
        )
    pair[0].wait_recv()
    mixed = partial_ref[...].astype(F32) + other_partial[...].astype(F32)
    total = tokens_ref[...].astype(F32) + mixed
    stream[0] = total[:, :HALF]
    stream[1] = total[:, HALF:]
    ffn_in = normalize(total, gain_ref[...])
    own_rows[0] = ffn_in[:, :HALF]
    own_rows[1] = ffn_in[:, HALF:]
    for d in range(1, RING):
        q = place * RING + lax.rem(x + d, RING)
        pending.append(
            send(own_rows.at[core], row_in.at[x], row_send.at[0, d], row_recv.at[0, d], q, core)
        )
    row_in[x] = own_rows[core]
    for d in range(1, RING):
        pending[d - 1].wait_recv()
        row = row + weight_in[d]
    weight_table[pl.ds(place, 1), :] = row
    for d in range(1, RING):
        pending[RING - 1 + d - 1].wait_recv()
    rows16 = jnp.concatenate([row_in[j].astype(F32) for j in range(RING)], axis=0)
    own_block = gathered.at[core, pl.ds(pl.multiple_of(place * BLOCK, BLOCK), BLOCK)]
    own_block[...] = rows16.astype(BF16)

    arriving = []
    for i, (dz, dy) in enumerate(OFFSETS):
        q = plane_at(dz, dy) * RING + x
        arriving.append(
            (
                send(own_block, own_block, plane_send.at[0, i], plane_recv.at[0, i], q, core),
                send(
                    weight_table.at[pl.ds(place, 1)],
                    weight_table.at[pl.ds(place, 1)],
                    plane_send.at[1, i],
                    plane_recv.at[1, i],
                    q,
                    core,
                ),
            )
        )
    shared = [send(own_block, own_block, share_send.at[PLANE - 1], share_recv.at[PLANE - 1], chip, other)]
    for i in reversed(range(PLANE - 1)):
        dz, dy = OFFSETS[i]
        arriving[i][0].wait_recv()
        came = plane_at(RING - dz, RING - dy)
        block = gathered.at[core, pl.ds(pl.multiple_of(came * BLOCK, BLOCK), BLOCK)]
        shared.append(send(block, block, share_send.at[i], share_recv.at[i], chip, other))

    for copy in loading[1:]:
        copy.wait()
    pair[1].wait_recv()
    for half in range(2):
        w_down[half, UNITS:, :] = (
            w_down[half, UNITS:, :].astype(F32) * scales[half]
        ).astype(BF16)
    for i in range(PLANE - 1):
        arriving[i][1].wait_recv()
    expert = chip // EXPERTS
    sub = lax.broadcasted_iota(jnp.int32, (BLOCK, 128), 0)
    lane16 = lax.broadcasted_iota(jnp.int32, (BLOCK, 128), 1)
    picked = lane16 == sub * EXPERTS + expert
    table = weight_table[...]
    columns = [
        jnp.sum(jnp.where(picked, table[g : g + 1, :], 0.0), axis=1, keepdims=True)
        for g in range(PLANE)
    ]
    column = jnp.concatenate(columns, axis=0)

    for copy in shared:
        copy.wait_recv()
    nt = (((1,), (1,)), ((), ()))
    raised = lax.dot_general(
        gathered[0], w_in[:, :HALF], nt, preferred_element_type=F32
    ) + lax.dot_general(gathered[1], w_in[:, HALF:], nt, preferred_element_type=F32)
    gated = raised[:, :ALL_UNITS]
    lifted = raised[:, ALL_UNITS:]
    unit = lax.broadcasted_iota(jnp.int32, (TOKENS, ALL_UNITS), 1)
    hidden = gated / (1.0 + jnp.exp(-gated)) * lifted * jnp.where(unit < UNITS, column, 1.0)
    hidden = hidden.astype(BF16)
    part_out[...] = jnp.dot(hidden, w_down[other], preferred_element_type=F32).astype(BF16)
    swap = send(part_out, part_in, sum_send.at[0], sum_recv.at[0], chip, other)
    part_own[...] = jnp.dot(hidden, w_down[core], preferred_element_type=F32)
    swap.wait_recv()
    summed = part_own[...] + part_in[...].astype(F32)
    block_out[...] = summed.astype(BF16)
    part_own[...] = summed
    back = []
    for i, (dz, dy) in enumerate(OFFSETS):
        q = plane_at(dz, dy)
        block = block_out.at[pl.ds(pl.multiple_of(q * BLOCK, BLOCK), BLOCK)]
        back.append(
            send(block, block_in.at[i], back_send.at[i], back_recv.at[i], q * RING + x, core)
        )
    total = part_own[pl.ds(pl.multiple_of(place * BLOCK, BLOCK), BLOCK), :]
    for i in reversed(range(PLANE - 1)):
        back[i].wait_recv()
        total = total + block_in[i].astype(F32)
    for j in range(RING):
        piece_out[j] = total[j * ROWS : (j + 1) * ROWS, :].astype(BF16)
    pieces = []
    for d in range(1, RING):
        at = lax.rem(x + d, RING)
        pieces.append(
            send(
                piece_out.at[at],
                piece_in.at[d],
                piece_send.at[d],
                piece_recv.at[d],
                place * RING + at,
                core,
            )
        )
    result = stream[core] + piece_out[x].astype(F32)
    for copy in pieces:
        copy.wait_recv()
    for d in range(1, RING):
        result = result + piece_in[d].astype(F32)
    out_ref[...] = result.astype(BF16)

    for copy in pair + pending + shared + [swap] + back + pieces:
        copy.wait_send()
    for a, b in arriving:
        a.wait_send()
        b.wait_send()


def cell_kernel(
    tokens_hbm,
    gain_hbm,
    w_gates_hbm,
    w_forget_hbm,
    bias_hbm,
    stabilizer_hbm,
    normalizer_hbm,
    query_hbm,
    key_hbm,
    value_hbm,
    memory_hbm,
    read_ref,
    new_memory_hbm,
    new_normalizer_ref,
    new_stabilizer_ref,
    tokens,
    gain,
    w_gates,
    w_forget,
    bias,
    stabilizer,
    normalizer,
    w_mixer,
    memory,
    turned,
    load_sem,
    store_sem,
):
    loads = [
        (tokens_hbm, tokens),
        (gain_hbm, gain),
        (query_hbm, w_mixer.at[0]),
        (w_gates_hbm, w_gates),
        (w_forget_hbm, w_forget),
        (bias_hbm, bias),
        (stabilizer_hbm, stabilizer),
        (normalizer_hbm, normalizer),
        (key_hbm, w_mixer.at[1]),
        (value_hbm, w_mixer.at[2]),
        *[(memory_hbm.at[i], memory.at[i]) for i in range(PAIRS)],
    ]
    loading = []
    for i, (src, dst) in enumerate(loads):
        copy = pltpu.make_async_copy(src, dst, load_sem.at[i])
        copy.start()
        loading.append(copy)
    loading[0].wait()
    loading[1].wait()
    normed = normalize(tokens[...], gain[...])

    def projected(i, at):
        loading[at].wait()
        return jnp.dot(normed, w_mixer[i], preferred_element_type=F32).astype(BF16).astype(F32)

    query = projected(0, 2)
    for i in range(3, 8):
        loading[i].wait()
    nt = (((1,), (1,)), ((), ()))
    in_gates = lax.dot_general(w_gates[...], normed, nt, preferred_element_type=F32)
    forgets = lax.dot_general(w_forget[...], normed, nt, preferred_element_type=F32)
    carries, admits, floors = [], [], []
    for h in range(HEADS):
        in_gate = in_gates[h : h + 1, :]
        forget_log = jax.nn.log_sigmoid(forgets[h : h + 1, :] + bias[:, h : h + 1])
        held = forget_log + stabilizer[h : h + 1, :]
        new_stabilizer = jnp.maximum(held, in_gate)
        new_stabilizer_ref[h : h + 1, :] = new_stabilizer
        carries.append(jnp.exp(held - new_stabilizer))
        admits.append(jnp.exp(in_gate - new_stabilizer))
        floors.append(jnp.exp(-new_stabilizer))
    key = projected(1, 8) * HEAD_SIZE ** (-0.5)
    turned[...] = jnp.concatenate([query, key], axis=0).T
    value = projected(2, 9)
    storing = []
    reads = [[None] * HEADS for _ in range(ROWS)]
    for t in range(ROWS):
        for h in range(HEADS):
            pair = t * HEADS + h
            part = slice(h * HEAD_SIZE, (h + 1) * HEAD_SIZE)
            carry = carries[h][:, t : t + 1]
            admit = admits[h][:, t : t + 1]
            updated = carry * normalizer[t, h : h + 1, :] + admit * key[t : t + 1, part]
            new_normalizer_ref[t, h : h + 1, :] = updated
            denom = jnp.sum(updated * query[t : t + 1, part], axis=1, keepdims=True)
            bound = jnp.maximum(jnp.abs(denom), floors[h][:, t : t + 1])
            values = admit * value[t : t + 1, part]
            loading[10 + pair].wait()

            def step(c, total, pair=pair, h=h, t=t, carry=carry, values=values):
                at = pl.multiple_of(c * CHUNK, CHUNK)
                sides = turned[pl.ds(pl.multiple_of(h * HEAD_SIZE + at, CHUNK), CHUNK), :]
                q, k = sides[:, t : t + 1], sides[:, ROWS + t : ROWS + t + 1]
                new = carry * memory[pair, pl.ds(at, CHUNK), :] + k * values
                memory[pair, pl.ds(at, CHUNK), :] = new
                return total + jnp.sum((q * new).reshape(CHUNK // 8, 8, HEAD_SIZE), axis=0)

            total = lax.fori_loop(
                0, HEAD_SIZE // CHUNK, step, jnp.zeros((8, HEAD_SIZE), F32)
            )
            reads[t][h] = jnp.sum(total, axis=0, keepdims=True) / bound
            copy = pltpu.make_async_copy(
                memory.at[pair], new_memory_hbm.at[pair], store_sem.at[pair]
            )
            copy.start()
            storing.append(copy)
    rows = [jnp.concatenate(r, axis=1) for r in reads]
    read_ref[...] = jnp.concatenate(rows, axis=0).astype(BF16)
    for copy in storing:
        copy.wait()


def cell_step(
    tokens,
    mixer_gain,
    w_input_gate,
    w_forget_gate,
    forget_bias,
    stabilizer,
    normalizer,
    w_query,
    w_key,
    w_value,
    memory,
):
    vmem = pl.BlockSpec(memory_space=pltpu.VMEM)
    hbm = pl.BlockSpec(memory_space=pltpu.HBM)
    operands = (
        tokens,
        mixer_gain.reshape(1, WIDTH),
        w_input_gate.T,
        w_forget_gate.T,
        forget_bias.reshape(1, HEADS),
        stabilizer.T,
        normalizer,
        w_query,
        w_key,
        w_value,
        memory.reshape(PAIRS, HEAD_SIZE, HEAD_SIZE),
    )
    read, new_memory, new_normalizer, new_stabilizer = pl.pallas_call(
        cell_kernel,
        out_shape=[
            jax.ShapeDtypeStruct((ROWS, WIDTH), BF16),
            pltpu.HBM((PAIRS, HEAD_SIZE, HEAD_SIZE), F32),
            jax.ShapeDtypeStruct((ROWS, HEADS, HEAD_SIZE), F32),
            jax.ShapeDtypeStruct((HEADS, ROWS), F32),
        ],
        in_specs=[hbm] * len(operands),
        out_specs=[vmem, hbm, vmem, vmem],
        scratch_shapes=[
            pltpu.VMEM((ROWS, WIDTH), BF16),
            pltpu.VMEM((1, WIDTH), F32),
            pltpu.VMEM((HEADS, WIDTH), BF16),
            pltpu.VMEM((HEADS, WIDTH), BF16),
            pltpu.VMEM((1, HEADS), F32),
            pltpu.VMEM((HEADS, ROWS), F32),
            pltpu.VMEM((ROWS, HEADS, HEAD_SIZE), F32),
            pltpu.VMEM((3, WIDTH, WIDTH), BF16),
            pltpu.VMEM((PAIRS, HEAD_SIZE, HEAD_SIZE), F32),
            pltpu.VMEM((WIDTH, 8), F32),
            pltpu.SemaphoreType.DMA((10 + PAIRS,)),
            pltpu.SemaphoreType.DMA((PAIRS,)),
        ],
        compiler_params=pltpu.CompilerParams(vmem_limit_bytes=K1_VMEM),
    )(*[pltpu.with_memory_space_constraint(a, pltpu.HBM) for a in operands])
    return read, new_memory.reshape(memory.shape), new_normalizer, new_stabilizer.T


def ffn(tokens, read, ffn_gain, ids, weights, scale, w_output, gate, up, down, dense_gate, dense_up, dense_down):
    vmem = pl.BlockSpec(memory_space=pltpu.VMEM)
    hbm = pl.BlockSpec(memory_space=pltpu.HBM)
    dma = pltpu.SemaphoreType.DMA
    return pl.pallas_call(
        ffn_kernel,
        out_shape=jax.ShapeDtypeStruct((ROWS, HALF), BF16),
        in_specs=[vmem] * 6 + [hbm] * 7,
        out_specs=vmem,
        scratch_shapes=[
            pltpu.VMEM((WIDTH, WIDTH), BF16),
            pltpu.VMEM((ROWS, WIDTH), BF16),
            pltpu.VMEM((ROWS, WIDTH), BF16),
            pltpu.VMEM((2, 1, HALF), F32),
            pltpu.VMEM((2, ROWS, HALF), F32),
            pltpu.VMEM((2, ROWS, HALF), BF16),
            pltpu.VMEM((RING, ROWS, HALF), BF16),
            pltpu.VMEM((1, 128), F32),
            pltpu.VMEM((RING, 1, 128), F32),
            pltpu.VMEM((2, TOKENS, HALF), BF16),
            pltpu.VMEM((PLANE, 128), F32),
            pltpu.VMEM((2 * ALL_UNITS, WIDTH), BF16),
            pltpu.VMEM((2, ALL_UNITS, HALF), BF16),
            pltpu.VMEM((TOKENS, HALF), BF16),
            pltpu.VMEM((TOKENS, HALF), BF16),
            pltpu.VMEM((TOKENS, HALF), F32),
            pltpu.VMEM((TOKENS, HALF), BF16),
            pltpu.VMEM((PLANE, BLOCK, HALF), BF16),
            pltpu.VMEM((RING, ROWS, HALF), BF16),
            pltpu.VMEM((RING, ROWS, HALF), BF16),
            dma((9,)),
            dma((2,)),
            dma((2,)),
            dma((2, RING)),
            dma((2, RING)),
            dma((2, PLANE)),
            dma((2, PLANE)),
            dma((PLANE,)),
            dma((PLANE,)),
            dma((1,)),
            dma((1,)),
            dma((PLANE,)),
            dma((PLANE,)),
            dma((RING,)),
            dma((RING,)),
        ],
        compiler_params=pltpu.CompilerParams(
            collective_id=0, has_side_effects=True, vmem_limit_bytes=K2_VMEM
        ),
    )(
        tokens,
        read,
        ffn_gain,
        ids,
        weights,
        scale,
        *[
            pltpu.with_memory_space_constraint(w, pltpu.HBM)
            for w in (w_output, gate, up, down, dense_gate, dense_up, dense_down)
        ],
    )


def shards(
    tokens,
    mixer_gain,
    w_query,
    w_key,
    w_value,
    w_input_gate,
    w_forget_gate,
    forget_bias,
    w_output,
    memory,
    normalizer,
    stabilizer,
    ffn_gain,
    route_ids,
    route_weights,
    expert_gate,
    expert_up,
    expert_down,
    dense_gate_w,
    dense_up_w,
    dense_down_w,
    dense_scale,
):
    read, new_memory, new_normalizer, new_stabilizer = cell_step(
        tokens,
        mixer_gain,
        w_input_gate,
        w_forget_gate,
        forget_bias,
        stabilizer,
        normalizer,
        w_query,
        w_key,
        w_value,
        memory,
    )
    output = ffn(
        tokens,
        read,
        ffn_gain.reshape(1, WIDTH),
        route_ids.T,
        route_weights.T,
        dense_scale.reshape(1, HALF),
        w_output,
        expert_gate[0].T,
        expert_up[0].T,
        expert_down[0],
        dense_gate_w.T,
        dense_up_w.T,
        dense_down_w,
    )
    return (output, new_memory, new_normalizer, new_stabilizer)


def solution(mesh):
    placed = (
        P("ep", None),
        P(),
        P(None, "tp"),
        P(None, "tp"),
        P(None, "tp"),
        P(None, "tp"),
        P(None, "tp"),
        P("tp"),
        P("tp", None),
        P("ep", "tp", None, None),
        P("ep", "tp", None),
        P("ep", "tp"),
        P(),
        P("ep", None),
        P("ep", None),
        P("ep", None, "tp"),
        P("ep", None, "tp"),
        P("ep", "tp", None),
        P(None, ("ep", "tp")),
        P(None, ("ep", "tp")),
        P(("ep", "tp"), None),
        P("tp"),
    )
    return jax.shard_map(
        shards,
        mesh=mesh,
        in_specs=placed,
        out_specs=(P("ep", "tp"), P("ep", "tp", None, None), P("ep", "tp", None), P("ep", "tp")),
        check_vma=False,
    )
```
